32 devices in a mesh: ep: 8 (over z, x), tp: 4 (over y, core).
Axes of the slice: x: 2, y: 2, z: 4, core: 2. Of those that a mesh axis runs over, the one named last changes fastest.
Arguments:
- queries: bfloat16 [8192, 2048], P('ep', 'tp'), may hold values from -128 to 128
- key_heads: bfloat16 [8192, 1024], P('ep', 'tp'), may hold values from -6 to 6
- value_heads: bfloat16 [8192, 1024], P('ep', 'tp'), may hold values from -6 to 6
- sink_logits: float32 [32], P('tp'), may hold values from 1 to 5
- mix_weight: bfloat16 [2048, 2048], replicated, may hold values from -1 to 1
- expert_input: bfloat16 [4096, 2048], P(('ep', 'tp')), may hold values from -6 to 6
- norm_gain: float32 [2048], replicated, may hold values from 0.1 to 1.9
- routes: int32 [4096, 4], P(('ep', 'tp')), may hold values from 0 to 31, all different within a row; in each aligned block of 128 rows (0 to 127, 128 to 255, ...) at most 32 rows name the same one
- route_weights: float32 [4096, 4], P(('ep', 'tp')), may hold values from 0.1 to 1
- gate_weight: bfloat16 [32, 2048, 1024], P(('ep', 'tp')), may hold values from -0.375 to 0.375
- up_weight: bfloat16 [32, 2048, 1024], P(('ep', 'tp')), may hold values from -0.375 to 0.375
- down_weight: bfloat16 [32, 1024, 2048], P(('ep', 'tp')), may hold values from -0.046875 to 0.046875
Outputs:
- mixer_out: bfloat16 [8192, 2048], P(('ep', 'tp'))
- experts_out: bfloat16 [4096, 2048], P(('ep', 'tp'))
The draws below stay inside these ranges and needn't reach their ends.
Inputs may be any that keep to these rules, and one draw needn't show every extreme that they name: `routes`: each row names 4 different experts; within the 128 rows of one device no expert is named more than 32 times, and in some devices' rows some expert is named exactly 32 times.
All inputs are finite; a program needn't handle non-finite values.
Results may differ from the reference program's by a relative error of at most 0.012.
The reference program's roundings to bfloat16 on the way count: a program that leaves them out, or rounds other values in their place, can miss the bound.
Values may be sent and summed in bfloat16 or wider, within the bound.
A program may use at most 128 MiB of HBM per device.

```python
import math
import jax
import jax.numpy as jnp
import numpy as np
from jax import lax

D = 2048
HEADS = 32
KV_HEADS = 16
HEAD_DIM = 64
WINDOW = 128
GRID_W = 64
FF = 1024
TOPK = 4
TOK_B = 128
TOKENS_A = 8192
TOKENS_B = 4096
EXPERTS = 32
CAP = 32
N_EP = 8
N_TP = 4


def query_key_pair(key):
    base_seed = jax.random.fold_in(key, 7)
    query_seed, key_seed = jax.random.split(base_seed, 2)
    length = TOKENS_A
    key_part = jnp.clip(jax.random.normal(key_seed, (length, KV_HEADS * HEAD_DIM), jnp.float32), -4.0, 4.0)
    query_part = jnp.clip(jax.random.normal(query_seed, (length, HEADS * HEAD_DIM), jnp.float32), -4.0, 4.0)
    return (query_part, key_part)


def draw_queries(key, part):
    return query_key_pair(key)[0].astype(jnp.bfloat16)


def draw_key_heads(key, part):
    return query_key_pair(key)[1].astype(jnp.bfloat16)


def level_of(own_key, extent, pieces, least, top_value):
    gain = 1.0
    for position, blocks in pieces:
        draws = jax.random.uniform(jax.random.fold_in(jax.random.fold_in(own_key, 6), position), (blocks,), jnp.float32, least / len(pieces), top_value / len(pieces))
        gain = gain * jnp.repeat(jnp.exp(draws), extent[position] // blocks).reshape((-1,) + (1,) * (len(extent) - 1 - position))
    return gain


def routed_block(stream_key, own, number, rows, number_of, top, bound, slope):
    sequence = jax.random.permutation(stream_key, number_of)
    heavy_load, usual = shares(number_of, rows * top, bound, slope, True), shares(number_of, rows * top, bound, slope, False)
    places = jnp.arange(number_of)

    def named(lengths, turn):
        used = int((lengths > 0).sum())
        fixed = max(1, used // 4)
        shifted = fixed + (places - fixed + turn * (used - fixed)) % max(1, number_of - fixed)
        return jnp.zeros((number_of,), jnp.int32).at[sequence[jnp.where(places < fixed, places, shifted)]].set(jnp.asarray(lengths, jnp.int32))

    lengths = jnp.where(number % 4 == 0, named(heavy_load, number // 4), named(usual, number - number // 4 - 1))
    mixed = jax.random.permutation(jax.random.fold_in(own, 3), number_of)
    giver, taker = mixed[0:number_of // 2 * 2:2], mixed[1:number_of // 2 * 2:2]
    room = jnp.minimum(lengths[giver] - 1, bound - lengths[taker]) // 2
    room = jnp.where((giver == sequence[0]) | (taker == sequence[0]) | (lengths[taker] == 0), 0, jnp.maximum(room, 0))
    shifted = jax.random.randint(jax.random.fold_in(own, 4), (number_of // 2,), 0, 1 << 20) % (room + 1)
    lengths = lengths.at[giver].add(-shifted).at[taker].add(shifted)
    items = jnp.searchsorted(jnp.cumsum(lengths), jnp.arange(rows * top), side="right").astype(jnp.int32)
    table = items.reshape(top, rows).T
    table = table[jax.random.permutation(jax.random.fold_in(own, 1), rows)]
    turn = jax.random.randint(jax.random.fold_in(own, 2), (rows, 1), 0, top)
    return jnp.take_along_axis(table, (jnp.arange(top)[None, :] + turn) % top, axis=1)


def shares(count, total, most, skew, full):
    loads = [(1 << 20) // math.isqrt(rank ** skew) + 1 for rank in range(1, count + 1)]
    largest = most if full else min(most, max(-(-total // count), total * loads[0] // sum(loads)))
    least = 1 if total - largest >= count - 1 else 0
    counts, rest = [largest] + [least] * (count - 1), total - largest - least * (count - 1)
    while rest > 0:
        candidates = [i for i in range(1, count) if counts[i] < largest] or [i for i in range(1, count) if counts[i] < most]
        whole, budget = sum([loads[i] for i in candidates]), rest
        for i in candidates:
            extra = min(most - counts[i], max(1, budget * loads[i] // whole), rest)
            counts[i] = counts[i] + extra
            rest = rest - extra
    return np.array(counts)


def scatter_about(key, extent, scale, reach, shards=(), kind=jnp.bfloat16):
    result = scale * jax.random.normal(key, extent, jnp.float32)
    if shards:
        result = result * level_of(key, extent, shards, -0.22, 0.18)
    return jnp.clip(result, -reach, reach).astype(kind)


def setup_inputs(seed: int = 0) -> dict:
    key_list = jax.random.split(jax.random.key(seed), 13)
    queries = draw_queries(jax.random.fold_in(key_list[12], 71), 0)
    key_heads = draw_key_heads(jax.random.fold_in(key_list[12], 71), 0)
    value_heads = scatter_about(key_list[2], (TOKENS_A, KV_HEADS * HEAD_DIM), 1.0, 6.0, ((0, 8), (1, 4)))
    sink_logits = jnp.clip(1.0 + 4.0 * jax.random.uniform(key_list[3], (HEADS,), jnp.float32) ** level_of(key_list[3], (HEADS,), ((0, 4),), -0.2, 0.2), 1.0, 5.0)
    mix_weight = scatter_about(key_list[4], (HEADS * HEAD_DIM, D), (HEADS * HEAD_DIM // 64) ** -0.5, 1.0)
    expert_input = scatter_about(key_list[5], (TOKENS_B, D), 1.0, 6.0, ((0, 32),))
    norm_gain = jnp.clip(1.0 + 0.18 * jax.random.normal(key_list[6], (D,), jnp.float32), 0.1, 1.9)
    routes_keys = jax.random.split(jax.random.fold_in(key_list[7], 1), TOKENS_B // TOK_B)
    routes_turns = jax.random.permutation(jax.random.fold_in(key_list[7], 3), TOKENS_B // TOK_B)
    routes = jax.vmap(lambda own, number: routed_block(jax.random.fold_in(key_list[7], 2), own, number, TOK_B, EXPERTS, TOPK, CAP, 2))(routes_keys, routes_turns).reshape((TOKENS_B, TOPK))
    route_weights = jnp.clip(jnp.exp(math.log(1.0) - 2.3025851 * jax.random.uniform(key_list[8], (TOKENS_B, TOPK), jnp.float32) ** level_of(key_list[8], (TOKENS_B, TOPK), ((0, 32),), -0.2, 0.2)), 0.1, 1.0)
    gate_weight = scatter_about(key_list[9], (EXPERTS, D, FF), (D // 9) ** -0.5, 0.375, ((0, 32),))
    up_weight = scatter_about(key_list[10], (EXPERTS, D, FF), (D // 9) ** -0.5, 0.375, ((0, 32),))
    down_weight = scatter_about(key_list[11], (EXPERTS, FF, D), (FF * 16) ** -0.5, 0.046875, ((0, 32),))
    return {"queries": queries, "key_heads": key_heads, "value_heads": value_heads, "sink_logits": sink_logits, "mix_weight": mix_weight, "expert_input": expert_input, "norm_gain": norm_gain, "routes": routes, "route_weights": route_weights, "gate_weight": gate_weight, "up_weight": up_weight, "down_weight": down_weight}


ROPE_BASE = 10000.0
CLAMP_LIMIT = 7.0
GATE_SLOPE = 1.702
NORM_EPS = 1e-05

def rotate_pairs(table, grid_rows, grid_cols, head_width):
    length = table.shape[0]
    quarter = head_width // 4
    shaped = table.reshape(length, -1, 2, 2, quarter)
    freqs = ROPE_BASE ** (-jnp.arange(0, head_width // 2, 2, dtype=jnp.float32) / (head_width // 2))
    angles = jnp.stack([grid_rows, grid_cols], axis=-1)[:, :, None] * freqs
    cosines = jnp.cos(angles)[:, None]
    sine_part = jnp.sin(angles)[:, None]
    former = shaped[..., 0, :]
    latter = shaped[..., 1, :]
    turned = jnp.stack([former * cosines - latter * sine_part, latter * cosines + former * sine_part], axis=-2)
    return turned.reshape(length, -1)

def grid_place(positions):
    return ((positions // GRID_W).astype(jnp.float32), (positions % GRID_W).astype(jnp.float32))

def attend(queries, key_heads, value_heads, sink_logits):
    length = queries.shape[0]
    group_size = HEADS // KV_HEADS
    positions = jnp.arange(length, dtype=jnp.int32)
    grid_rows, grid_cols = grid_place(positions)
    q_rot = rotate_pairs(queries.astype(jnp.float32), grid_rows, grid_cols, HEAD_DIM).astype(jnp.bfloat16)
    k_rot = rotate_pairs(key_heads.astype(jnp.float32), grid_rows, grid_cols, HEAD_DIM).astype(jnp.bfloat16)
    k_padded = jnp.pad(k_rot, ((WINDOW, WINDOW), (0, 0)))
    v_padded = jnp.pad(value_heads, ((WINDOW, WINDOW), (0, 0)))
    block_rows = math.gcd(length, 512)
    key_span = block_rows + 2 * WINDOW
    sink_grid = sink_logits.astype(jnp.float32).reshape(KV_HEADS, group_size)

    def one_block(block_index):
        first_row = block_index * block_rows
        q_blk = lax.dynamic_slice_in_dim(q_rot, first_row, block_rows, 0).astype(jnp.float32)
        q_blk = q_blk.reshape(block_rows, KV_HEADS, group_size, HEAD_DIM)
        k_blk = lax.dynamic_slice_in_dim(k_padded, first_row, key_span, 0).astype(jnp.float32)
        k_blk = k_blk.reshape(key_span, KV_HEADS, HEAD_DIM)
        v_blk = lax.dynamic_slice_in_dim(v_padded, first_row, key_span, 0).astype(jnp.float32)
        v_blk = v_blk.reshape(key_span, KV_HEADS, HEAD_DIM)
        q_pos = first_row + jnp.arange(block_rows, dtype=jnp.int32)
        k_pos = first_row - WINDOW + jnp.arange(key_span, dtype=jnp.int32)
        inside = (jnp.abs(q_pos[:, None] - k_pos[None, :]) <= WINDOW) & (k_pos >= 0) & (k_pos < length)
        scores = jnp.einsum('qkgd,skd->kgqs', q_blk, k_blk) * HEAD_DIM ** (-0.5)
        scores = jnp.where(inside, scores, -jnp.inf)
        peak = jnp.maximum(lax.optimization_barrier(jnp.max(scores, axis=-1)), sink_grid[:, :, None])
        weights_exp = jnp.exp(scores - peak[..., None])
        denominator = lax.optimization_barrier(jnp.sum(weights_exp, axis=-1)) + jnp.exp(sink_grid[:, :, None] - peak)
        chances = (weights_exp / denominator[..., None]).astype(jnp.bfloat16)
        blended = jnp.einsum('kgqs,skd->qkgd', chances.astype(jnp.float32), v_blk)
        return blended.astype(jnp.bfloat16).reshape(block_rows, HEADS * HEAD_DIM)
    blocks = lax.map(one_block, jnp.arange(length // block_rows, dtype=jnp.int32))
    return blocks.reshape(length, HEADS * HEAD_DIM)

def normalize(tokens_in, gain_row):
    values = tokens_in.astype(jnp.float32)
    center = lax.optimization_barrier(jnp.mean(values, axis=-1, keepdims=True))
    spread = lax.optimization_barrier(jnp.mean(jnp.square(values - center), axis=-1, keepdims=True))
    return ((values - center) * lax.rsqrt(spread + NORM_EPS) * gain_row.astype(jnp.float32)).astype(jnp.bfloat16)

def expert_rows(row_block, w_gate, w_lift, w_down):
    gate_pre = jnp.dot(row_block, w_gate, preferred_element_type=jnp.float32)
    lift_pre = jnp.dot(row_block, w_lift, preferred_element_type=jnp.float32)
    gate_pre = jnp.minimum(gate_pre, CLAMP_LIMIT)
    lift_pre = jnp.clip(lift_pre, -CLAMP_LIMIT, CLAMP_LIMIT)
    activated = ((lift_pre + 1.0) * gate_pre * jax.nn.sigmoid(GATE_SLOPE * gate_pre)).astype(jnp.bfloat16)
    return jnp.dot(activated, w_down, preferred_element_type=jnp.float32).astype(jnp.bfloat16)

def slot_within(route_block):
    flat_routes = route_block.reshape(-1)
    matches = (flat_routes[:, None] == jnp.arange(EXPERTS, dtype=jnp.int32)[None, :]).astype(jnp.int32)
    earlier = jnp.cumsum(matches, axis=0) - matches
    return lax.optimization_barrier(jnp.sum(earlier * matches, axis=1)).astype(jnp.int32)

def reference(queries, key_heads, value_heads, sink_logits, mix_weight, expert_input, norm_gain, routes, route_weights, gate_weight, up_weight, down_weight):
    attended = attend(queries, key_heads, value_heads, sink_logits)
    mixer_out = jnp.dot(attended, mix_weight, preferred_element_type=jnp.float32).astype(jnp.bfloat16)
    sources = N_EP * N_TP
    normed = normalize(expert_input, norm_gain)
    slots = jax.vmap(slot_within)(routes.reshape(sources, TOK_B, TOPK)).reshape(-1)
    flat_routes = routes.reshape(-1).astype(jnp.int32)
    token_of = (jnp.arange(TOKENS_B * TOPK, dtype=jnp.int32) // TOPK).astype(jnp.int32)
    source_of = (token_of // TOK_B).astype(jnp.int32)
    columns = (source_of * CAP + slots).astype(jnp.int32)
    table = jnp.full((EXPERTS, sources * CAP), TOKENS_B, jnp.int32).at[flat_routes, columns].set(token_of)
    padded_in = jnp.concatenate([normed, jnp.zeros((1, D), jnp.bfloat16)], axis=0)

    def one_expert(bundle):
        row_ids, w_gate, w_lift, w_down = bundle
        return expert_rows(padded_in[row_ids], w_gate, w_lift, w_down)
    results = lax.map(one_expert, (table, gate_weight, up_weight, down_weight))
    picked = results[flat_routes, columns].reshape(TOKENS_B, TOPK, D)
    summed = lax.optimization_barrier(jnp.sum(route_weights.astype(jnp.float32)[..., None] * picked.astype(jnp.float32), axis=1))
    return (mixer_out, summed.astype(jnp.bfloat16))
```

```python
import functools
import math

import jax
import jax.numpy as jnp
from jax import lax
from jax.experimental import pallas as pl
from jax.experimental.pallas import tpu as pltpu
from jax.sharding import Mesh
from jax.sharding import PartitionSpec as P

HEAD_DIM = 64
WINDOW = 128
GRID_W = 64
ROPE_BASE = 10000.0
CLAMP_LIMIT = 7.0
GATE_SLOPE = 1.702
NORM_EPS = 1e-05

F32 = jnp.float32
BF16 = jnp.bfloat16


def angle_tables(first, rows):
    half = HEAD_DIM // 2
    quarter = HEAD_DIM // 4
    positions = first + jnp.arange(rows, dtype=jnp.int32)
    lane = jnp.arange(2 * HEAD_DIM, dtype=jnp.int32) % HEAD_DIM
    freqs = ROPE_BASE ** (-jnp.arange(0, half, 2, dtype=F32) / half)
    lane_freq = jnp.tile(freqs, 2 * HEAD_DIM // quarter)
    by_row = (positions // GRID_W).astype(F32)[:, None]
    by_col = (positions % GRID_W).astype(F32)[:, None]
    angle = jnp.where((lane < half)[None, :], by_row, by_col) * lane_freq[None, :]
    sign = jnp.where(lane % half < quarter, -1.0, 1.0).astype(F32)
    return jnp.cos(angle), jnp.sin(angle) * sign[None, :]


def turn(cells, cosines, sines):
    quarter = HEAD_DIM // 4
    width = cells.shape[1]
    lane = lax.broadcasted_iota(jnp.int32, cells.shape, 1)
    ahead = pltpu.roll(cells, width - quarter, 1)
    behind = pltpu.roll(cells, quarter, 1)
    partner = jnp.where(lane % (2 * quarter) < quarter, ahead, behind)
    return cells * cosines + partner * sines


def attention_kernel(
    length, info, sink, q_ref, k_ref, v_ref, left_ref, right_ref, cos_ref, sin_ref, out_ref, k_scr, v_scr
):
    block = pl.program_id(0)
    rows_here = k_ref.shape[0]
    kv_local = k_scr.shape[0]
    bq = q_ref.shape[0]
    span = bq + 2 * WINDOW

    @pl.when(block == 0)
    def _():
        def place(source, values, start, count):
            for pair in range(kv_local // 2):
                cols = slice(pair * 128, pair * 128 + 128)
                turned = turn(
                    source[:, cols].astype(F32),
                    cos_ref[start : start + count, :],
                    sin_ref[start : start + count, :],
                ).astype(BF16)
                part = values[:, cols]
                for side in range(2):
                    k_scr[2 * pair + side, start : start + count, :] = turned[:, side * 64 : side * 64 + 64]
                    v_scr[2 * pair + side, start : start + count, :] = part[:, side * 64 : side * 64 + 64]

        place(left_ref[0], left_ref[1], 0, WINDOW)
        place(right_ref[0], right_ref[1], WINDOW + rows_here, WINDOW)
        for piece in range(rows_here // 256):
            at = piece * 256
            place(k_ref[at : at + 256, :], v_ref[at : at + 256, :], WINDOW + at, 256)

    first = pl.multiple_of(block * bq, bq)
    cosines = cos_ref[pl.ds(first + WINDOW, bq), :] * HEAD_DIM**-0.5
    sines = sin_ref[pl.ds(first + WINDOW, bq), :] * HEAD_DIM**-0.5
    row = lax.broadcasted_iota(jnp.int32, (2 * bq, span), 0) % bq
    col = lax.broadcasted_iota(jnp.int32, (2 * bq, span), 1)
    key_pos = info[0] + first - WINDOW + col
    inside = (col >= row) & (col <= row + 2 * WINDOW) & (key_pos >= 0) & (key_pos < length)
    top = lax.broadcasted_iota(jnp.int32, (2 * bq, 1), 0) < bq
    for g in range(kv_local):
        q = turn(q_ref[:, g * 128 : g * 128 + 128].astype(F32), cosines, sines).astype(BF16)
        q2 = jnp.concatenate([q[:, :64], q[:, 64:]], axis=0)
        k = k_scr[g, pl.ds(first, span), :]
        v = v_scr[g, pl.ds(first, span), :]
        scores = lax.dot_general(q2, k, (((1,), (1,)), ((), ())), preferred_element_type=F32)
        scores = jnp.where(inside, scores, -jnp.inf)
        logit = jnp.where(top, sink[2 * g], sink[2 * g + 1])
        peak = jnp.maximum(jnp.max(scores, axis=1, keepdims=True), logit)
        weights = jnp.exp(scores - peak)
        total = jnp.sum(weights, axis=1, keepdims=True) + jnp.exp(logit - peak)
        chances = (weights * (1.0 / total)).astype(BF16)
        blend = jnp.dot(chances, v, preferred_element_type=F32).astype(BF16)
        out_ref[:, g * 128 : g * 128 + 128] = jnp.concatenate([blend[:bq], blend[bq:]], axis=1)


def attention(queries, keys, values, left, right, cosines, sines, sink, first, length):
    rows, width = queries.shape
    kv_local = keys.shape[1] // HEAD_DIM
    bq = 128
    whole = pl.BlockSpec(memory_space=pltpu.VMEM)
    smem = pl.BlockSpec(memory_space=pltpu.SMEM)
    return pl.pallas_call(
        functools.partial(attention_kernel, length),
        grid=(rows // bq,),
        in_specs=[smem, smem, pl.BlockSpec((bq, width), lambda i: (i, 0))] + [whole] * 6,
        out_specs=pl.BlockSpec((bq, width), lambda i: (i, 0)),
        out_shape=jax.ShapeDtypeStruct((rows, width), BF16),
        scratch_shapes=[
            pltpu.VMEM((kv_local, rows + 2 * WINDOW, HEAD_DIM), BF16),
            pltpu.VMEM((kv_local, rows + 2 * WINDOW, HEAD_DIM), BF16),
        ],
        compiler_params=pltpu.CompilerParams(vmem_limit_bytes=32 * 1024 * 1024),
        cost_estimate=pl.CostEstimate(
            flops=rows * width * 384 * 4 * 8,
            bytes_accessed=rows * width * 8,
            transcendentals=rows * width * 6,
        ),
        name="attention",
    )(first, sink, queries, keys, values, left, right, cosines, sines)


def normalize(tokens_in, gain_row):
    values = tokens_in.astype(F32)
    center = jnp.mean(values, axis=-1, keepdims=True)
    spread = jnp.mean(jnp.square(values - center), axis=-1, keepdims=True)
    return ((values - center) * lax.rsqrt(spread + NORM_EPS) * gain_row).astype(BF16)


def ffn(row_block, w_gate, w_lift, w_down):
    gate_pre = jnp.dot(row_block, w_gate, preferred_element_type=F32)
    lift_pre = jnp.dot(row_block, w_lift, preferred_element_type=F32)
    gate_pre = jnp.minimum(gate_pre, CLAMP_LIMIT)
    lift_pre = jnp.clip(lift_pre, -CLAMP_LIMIT, CLAMP_LIMIT)
    activated = ((lift_pre + 1.0) * gate_pre * jax.nn.sigmoid(GATE_SLOPE * gate_pre)).astype(BF16)
    return jnp.dot(activated, w_down, preferred_element_type=F32).astype(BF16)


def body(
    queries,
    key_heads,
    value_heads,
    sink_logits,
    mix_weight,
    expert_input,
    norm_gain,
    routes,
    route_weights,
    gate_weight,
    up_weight,
    down_weight,
):
    n_z, n_x, n_tp = lax.axis_size("zz"), lax.axis_size("xx"), lax.axis_size("tp")
    n_ep = n_z * n_x
    experts = n_ep * n_tp
    plane = n_x * n_tp
    ep = lax.axis_index(("zz", "xx"))
    rows_here = queries.shape[0]
    tok, top_count = routes.shape
    capacity = 2 * tok * top_count // experts
    width = expert_input.shape[1]

    normed = normalize(expert_input, norm_gain)
    routing = jnp.concatenate([routes.astype(F32), route_weights], axis=1)
    routing = lax.all_gather(routing, "zz", axis=0)
    gathered = lax.all_gather(normed, "zz", axis=0)

    paired = jnp.stack([key_heads, value_heads])
    left = lax.ppermute(
        paired[:, rows_here - WINDOW :], ("zz", "xx"), [(i, i + 1) for i in range(n_ep - 1)]
    )
    right = lax.ppermute(paired[:, :WINDOW], ("zz", "xx"), [(i + 1, i) for i in range(n_ep - 1)])

    first_expert = lax.axis_index("zz") * plane
    named = routing[:, :, :top_count].astype(jnp.int32) - first_expert
    shares = routing[:, :, top_count:]
    here = named[:, :, :, None] == jnp.arange(plane, dtype=jnp.int32)
    member = jnp.any(here, axis=2)
    share = jnp.sum(jnp.where(here, shares[..., None], 0.0), axis=2)
    lower = jnp.tril(jnp.ones((tok, tok), BF16), -1)
    slot = jnp.einsum("ut,ztl->zul", lower, member.astype(BF16), preferred_element_type=F32)
    slot = jnp.where(member, slot.astype(jnp.int32), -1)
    chosen = slot[:, :, :, None] == jnp.arange(capacity, dtype=jnp.int32)
    pick = chosen.astype(BF16).reshape(n_z, tok, plane * capacity)
    outgoing = jnp.einsum("ztj,ztd->zjd", pick, gathered, preferred_element_type=F32).astype(BF16)
    outgoing = outgoing.reshape(n_z, plane, capacity, width).transpose(1, 0, 2, 3)
    arrived = lax.all_to_all(outgoing, ("xx", "tp"), split_axis=0, concat_axis=0, tiled=True)

    first = ep * rows_here
    cosines, sines = angle_tables(first - WINDOW, rows_here + 2 * WINDOW)
    attended = attention(
        queries,
        key_heads,
        value_heads,
        left,
        right,
        cosines,
        sines,
        sink_logits,
        first[None].astype(jnp.int32),
        rows_here * n_ep,
    )
    columns = attended.shape[1]
    token_rows = lax.all_to_all(
        attended.reshape(n_tp, rows_here // n_tp, columns), "tp", split_axis=0, concat_axis=0, tiled=True
    )

    produced = ffn(arrived.reshape(plane * n_z * capacity, width), gate_weight[0], up_weight[0], down_weight[0])
    produced = produced.reshape(plane, n_z, capacity, width)
    returned = lax.all_to_all(produced, ("xx", "tp"), split_axis=0, concat_axis=0, tiled=True)

    mixer_out = jnp.einsum(
        "trc,tcd->rd", token_rows, mix_weight.reshape(n_tp, columns, -1), preferred_element_type=F32
    ).astype(BF16)

    scaled = jnp.where(chosen, share[..., None], 0.0).reshape(n_z, tok, plane, capacity)
    coarse = scaled.astype(BF16)
    fine = (scaled - coarse.astype(F32)).astype(BF16)
    partial = jnp.einsum("ztls,lzsd->ztd", coarse, returned, preferred_element_type=F32)
    partial = partial + jnp.einsum("ztls,lzsd->ztd", fine, returned, preferred_element_type=F32)
    home = lax.all_to_all(partial.astype(BF16), "zz", split_axis=0, concat_axis=0, tiled=True)
    return mixer_out, jnp.sum(home.astype(F32), axis=0).astype(BF16)


def z_count(mesh, n_ep):
    coords = {getattr(d, "coords", (0, 0, 0))[2] for d in mesh.devices.flat}
    return len(coords) if n_ep % len(coords) == 0 else 1


def solution(mesh):
    n_ep, n_tp = mesh.shape["ep"], mesh.shape["tp"]
    n_z = z_count(mesh, n_ep)
    grid = Mesh(mesh.devices.reshape(n_z, n_ep // n_z, n_tp), ("zz", "xx", "tp"))
    ep = ("zz", "xx")
    every = ("zz", "xx", "tp")
    return jax.shard_map(
        body,
        mesh=grid,
        in_specs=(
            P(ep, "tp"),
            P(ep, "tp"),
            P(ep, "tp"),
            P("tp"),
            P(),
            P(every, None),
            P(),
            P(every, None),
            P(every, None),
            P(every, None, None),
            P(every, None, None),
            P(every, None, None),
        ),
        out_specs=(P(every, None), P(every, None)),
        check_vma=False,
    )
```

```python
import functools
import math

import jax
import jax.numpy as jnp
from jax import lax
from jax.experimental import pallas as pl
from jax.experimental.pallas import tpu as pltpu
from jax.sharding import Mesh
from jax.sharding import PartitionSpec as P

HEAD_DIM = 64
WINDOW = 128
GRID_W = 64
ROPE_BASE = 10000.0
CLAMP_LIMIT = 7.0
GATE_SLOPE = 1.702
NORM_EPS = 1e-05

F32 = jnp.float32
BF16 = jnp.bfloat16


def angle_tables(first, rows):
    half = HEAD_DIM // 2
    quarter = HEAD_DIM // 4
    positions = first + jnp.arange(rows, dtype=jnp.int32)
    lane = jnp.arange(2 * HEAD_DIM, dtype=jnp.int32) % HEAD_DIM
    freqs = ROPE_BASE ** (-jnp.arange(0, half, 2, dtype=F32) / half)
    lane_freq = jnp.tile(freqs, 2 * HEAD_DIM // quarter)
    by_row = (positions // GRID_W).astype(F32)[:, None]
    by_col = (positions % GRID_W).astype(F32)[:, None]
    angle = jnp.where((lane < half)[None, :], by_row, by_col) * lane_freq[None, :]
    sign = jnp.where(lane % half < quarter, -1.0, 1.0).astype(F32)
    return jnp.cos(angle), jnp.sin(angle) * sign[None, :]


def turn(cells, cosines, sines):
    quarter = HEAD_DIM // 4
    width = cells.shape[1]
    lane = lax.broadcasted_iota(jnp.int32, cells.shape, 1)
    ahead = pltpu.roll(cells, width - quarter, 1)
    behind = pltpu.roll(cells, quarter, 1)
    partner = jnp.where(lane % (2 * quarter) < quarter, ahead, behind)
    return cells * cosines + partner * sines

MESH = pl.DeviceIdType.MESH


def kernel(
    sizes,
    sink,
    route_ref,
    x_ref,
    gain_ref,
    q_ref,
    k_ref,
    v_ref,
    cos_ref,
    sin_ref,
    wg_hbm,
    wu_hbm,
    wd_hbm,
    mix_hbm,
    mixer_ref,
    expert_ref,
    k_scr,
    v_scr,
    halo,
    att,
    att_in,
    routing,
    normed,
    outgoing,
    arrived,
    produced,
    returned,
    shares,
    partial,
    home,
    wg,
    wu,
    wd,
    mix,
    act,
    z_send,
    z_recv,
    rt_send,
    rt_recv,
    out_send,
    out_recv,
    back_send,
    back_recv,
    home_send,
    home_recv,
    att_send,
    att_recv,
    halo_send,
    halo_recv,
    load_sem,
):
    n_z, n_x, n_tp, top_count, capacity = sizes
    n_ep = n_z * n_x
    plane = n_x * n_tp
    slots = plane * capacity
    z, x, t = lax.axis_index("zz"), lax.axis_index("xx"), lax.axis_index("tp")
    me = x * n_tp + t
    ep = z * n_x + x
    rows_here, width_q = q_ref.shape
    tok, width = x_ref.shape
    length = rows_here * n_ep
    kv_local = k_scr.shape[0]
    bq = WINDOW
    span = bq + 2 * WINDOW
    blocks = rows_here // bq
    chunk = rows_here // n_tp

    def z_dev(b):
        return (b, x, t)

    def plane_dev(p):
        return (z, lax.div(p, n_tp), lax.rem(p, n_tp))

    def ep_dev(e):
        return (lax.div(e, n_x), lax.rem(e, n_x), t)

    after, before = lax.rem(ep + 1, n_ep), lax.rem(ep + n_ep - 1, n_ep)

    loads = [
        pltpu.make_async_copy(wg_hbm.at[0], wg, load_sem.at[0]),
        pltpu.make_async_copy(wu_hbm.at[0], wu, load_sem.at[1]),
        pltpu.make_async_copy(wd_hbm.at[0], wd, load_sem.at[2]),
        pltpu.make_async_copy(mix_hbm, mix, load_sem.at[3]),
    ]
    for load in loads:
        load.start()

    barrier = pltpu.get_barrier_semaphore()

    def greet_z(o, _):
        pl.semaphore_signal(barrier, inc=1, device_id=z_dev(lax.rem(z + o, n_z)), device_id_type=MESH)
        return 0

    def greet_plane(p, _):
        pl.semaphore_signal(
            barrier, inc=1, device_id=plane_dev(lax.rem(me + p, plane)), device_id_type=MESH
        )
        return 0

    lax.fori_loop(1, n_z, greet_z, 0)
    lax.fori_loop(1, plane, greet_plane, 0)
    for e in (after, before):
        pl.semaphore_signal(barrier, inc=1, device_id=ep_dev(e), device_id_type=MESH)

    for part in range(tok // 32):
        rows = slice(part * 32, part * 32 + 32)
        values = x_ref[rows, :].astype(F32)
        center = jnp.mean(values, axis=1, keepdims=True)
        spread = jnp.mean(jnp.square(values - center), axis=1, keepdims=True)
        normed[z, rows, :] = (
            (values - center) * lax.rsqrt(spread + NORM_EPS) * gain_ref[...]
        ).astype(BF16)
    routing[z] = route_ref[...]
    pl.semaphore_wait(barrier, n_z - 1 + plane - 1 + 2)

    def rt_copy(o):
        return pltpu.make_async_remote_copy(
            src_ref=routing.at[z],
            dst_ref=routing.at[z],
            send_sem=rt_send.at[o],
            recv_sem=rt_recv.at[z],
            device_id=z_dev(lax.rem(z + o, n_z)),
            device_id_type=MESH,
        )

    def z_copy(o):
        return pltpu.make_async_remote_copy(
            src_ref=normed.at[z],
            dst_ref=normed.at[z],
            send_sem=z_send.at[o],
            recv_sem=z_recv.at[z],
            device_id=z_dev(lax.rem(z + o, n_z)),
            device_id_type=MESH,
        )

    def halo_copy(source, which, start, target):
        return pltpu.make_async_remote_copy(
            src_ref=source.at[pl.ds(start, WINDOW)],
            dst_ref=halo.at[which],
            send_sem=halo_send.at[which],
            recv_sem=halo_recv.at[which],
            device_id=ep_dev(target),
            device_id_type=MESH,
        )

    halos = [
        halo_copy(k_ref, 0, rows_here - WINDOW, after),
        halo_copy(v_ref, 1, rows_here - WINDOW, after),
        halo_copy(k_ref, 2, 0, before),
        halo_copy(v_ref, 3, 0, before),
    ]
    for o in range(1, n_z):
        rt_copy(o).start()
    for copy in halos:
        copy.start()
    for o in range(1, n_z):
        z_copy(o).start()

    def await_bytes(ref, sem):
        pltpu.make_async_copy(ref, ref, sem).wait()

    def source_of(o):
        return lax.rem(z + n_z - o, n_z)

    slot_row = lax.broadcasted_iota(jnp.int32, (slots, tok), 0)
    lane_expert = (z * plane + lax.div(slot_row, capacity)).astype(F32)
    place_in = lax.rem(slot_row, capacity).astype(F32)
    upper = (
        lax.broadcasted_iota(jnp.int32, (tok, tok), 0) < lax.broadcasted_iota(jnp.int32, (tok, tok), 1)
    ).astype(F32).astype(BF16)

    def dispatch(o):
        b = source_of(o)
        if o > 0:
            await_bytes(routing.at[b], rt_recv.at[b])
            await_bytes(normed.at[b], z_recv.at[b])
        route = routing[b]
        member = jnp.zeros((slots, tok), F32)
        share = jnp.zeros((slots, tok), F32)
        for k in range(top_count):
            hit = route[k : k + 1, :] == lane_expert
            member = jnp.where(hit, 1.0, member)
            share = jnp.where(hit, route[top_count + k : top_count + k + 1, :], share)
        rank = jnp.dot(member.astype(BF16), upper, preferred_element_type=F32)
        pick = jnp.where(rank == place_in, member, 0.0)
        scaled = (share * pick).T
        coarse = scaled.astype(BF16)
        shares[b, 0] = coarse
        shares[b, 1] = (scaled - coarse.astype(F32)).astype(BF16)
        pick = pick.astype(BF16)

        def tile(j, _):
            cols = pl.ds(pl.multiple_of(j * 256, 256), 256)
            outgoing[b, :, cols] = jnp.dot(
                pick, normed[b, :, cols], preferred_element_type=F32
            ).astype(BF16)
            return 0

        lax.fori_loop(0, width // 256, tile, 0)
        exchange(outgoing, arrived, out_send, out_recv, b)

    def exchange(source, target, send, recv, b):
        mine = pl.ds(pl.multiple_of(me * capacity, capacity), capacity)

        def one(p, _):
            to = lax.rem(me + p, plane)
            pltpu.make_async_remote_copy(
                src_ref=source.at[b, pl.ds(pl.multiple_of(to * capacity, capacity), capacity)],
                dst_ref=target.at[b, mine],
                send_sem=send.at[b],
                recv_sem=recv.at[b],
                device_id=plane_dev(to),
                device_id_type=MESH,
            ).start()
            return 0

        lax.fori_loop(1, plane, one, 0)
        pltpu.make_async_copy(source.at[b, mine], target.at[b, mine], recv.at[b]).start()

    def place(source, values, at, count):
        for pair in range(kv_local // 2):
            cols = slice(pair * 128, pair * 128 + 128)
            turned = turn(
                source[:, cols].astype(F32), cos_ref[pl.ds(at, count), :], sin_ref[pl.ds(at, count), :]
            ).astype(BF16)
            piece = values[:, cols]
            for side in range(2):
                lanes = slice(side * 64, side * 64 + 64)
                k_scr[2 * pair + side, pl.ds(at, count), :] = turned[:, lanes]
                v_scr[2 * pair + side, pl.ds(at, count), :] = piece[:, lanes]

    def place_own(i, _):
        at = pl.multiple_of(i * 128, 128)
        place(k_ref[pl.ds(at, 128), :], v_ref[pl.ds(at, 128), :], WINDOW + at, 128)
        return 0

    row = lax.rem(lax.broadcasted_iota(jnp.int32, (2 * bq, span), 0), bq)
    col = lax.broadcasted_iota(jnp.int32, (2 * bq, span), 1)
    top = lax.broadcasted_iota(jnp.int32, (2 * bq, 1), 0) < bq

    def attend(block, _):
        first = pl.multiple_of(block * bq, bq)
        cosines = cos_ref[pl.ds(first + WINDOW, bq), :] * HEAD_DIM**-0.5
        sines = sin_ref[pl.ds(first + WINDOW, bq), :] * HEAD_DIM**-0.5
        key_pos = ep * rows_here + first - WINDOW + col
        inside = (col >= row) & (col <= row + 2 * WINDOW) & (key_pos >= 0) & (key_pos < length)
        for g in range(kv_local):
            q = q_ref[pl.ds(first, bq), g * 128 : g * 128 + 128].astype(F32)
            q = turn(q, cosines, sines).astype(BF16)
            q2 = jnp.concatenate([q[:, :64], q[:, 64:]], axis=0)
            k = k_scr[g, pl.ds(first, span), :]
            v = v_scr[g, pl.ds(first, span), :]
            scores = lax.dot_general(q2, k, (((1,), (1,)), ((), ())), preferred_element_type=F32)
            scores = jnp.where(inside, scores, -jnp.inf)
            logit = jnp.where(top, sink[2 * g], sink[2 * g + 1])
            peak = jnp.maximum(jnp.max(scores, axis=1, keepdims=True), logit)
            weights = jnp.exp(scores - peak)
            total = jnp.sum(weights, axis=1, keepdims=True) + jnp.exp(logit - peak)
            chances = (weights * (1.0 / total)).astype(BF16)
            blend = jnp.dot(chances, v, preferred_element_type=F32).astype(BF16)
            att[pl.ds(first, bq), g * 128 : g * 128 + 128] = jnp.concatenate(
                [blend[:bq], blend[bq:]], axis=1
            )
        return 0

    def send_heads():
        def one(p, _):
            to = lax.rem(t + p, n_tp)
            pltpu.make_async_remote_copy(
                src_ref=att.at[pl.ds(pl.multiple_of(to * chunk, chunk), chunk)],
                dst_ref=att_in.at[t],
                send_sem=att_send,
                recv_sem=att_recv,
                device_id=(z, x, to),
                device_id_type=MESH,
            ).start()
            return 0

        lax.fori_loop(1, n_tp, one, 0)
        own = pl.ds(pl.multiple_of(t * chunk, chunk), chunk)
        pltpu.make_async_copy(att.at[own], att_in.at[t], att_recv).start()

    def experts(o):
        b = source_of(o)
        await_bytes(arrived.at[b], out_recv.at[b])
        hidden = wg.shape[1]

        def up(j, _):
            cols = pl.ds(pl.multiple_of(j * 256, 256), 256)
            rows = arrived[b]
            gate = jnp.dot(rows, wg[:, cols], preferred_element_type=F32)
            lift = jnp.dot(rows, wu[:, cols], preferred_element_type=F32)
            gate = jnp.minimum(gate, CLAMP_LIMIT)
            lift = jnp.clip(lift, -CLAMP_LIMIT, CLAMP_LIMIT)
            act[:, cols] = ((lift + 1.0) * gate * jax.nn.sigmoid(GATE_SLOPE * gate)).astype(BF16)
            return 0

        def down(j, _):
            cols = pl.ds(pl.multiple_of(j * 256, 256), 256)
            produced[b, :, cols] = jnp.dot(
                act[...], wd[:, cols], preferred_element_type=F32
            ).astype(BF16)
            return 0

        lax.fori_loop(0, hidden // 256, up, 0)
        lax.fori_loop(0, width // 256, down, 0)
        exchange(produced, returned, back_send, back_recv, b)

    def combine(o):
        b = source_of(o)
        await_bytes(returned.at[b], back_recv.at[b])

        def tile(j, _):
            cols = pl.ds(pl.multiple_of(j * 256, 256), 256)
            rows = returned[b, :, cols]
            total = jnp.dot(shares[b, 0], rows, preferred_element_type=F32)
            total = total + jnp.dot(shares[b, 1], rows, preferred_element_type=F32)
            partial[o, :, cols] = total.astype(BF16)
            return 0

        lax.fori_loop(0, width // 256, tile, 0)
        if o > 0:
            home_copy(o).start()

    def home_copy(o):
        return pltpu.make_async_remote_copy(
            src_ref=partial.at[o],
            dst_ref=home.at[o],
            send_sem=home_send.at[o],
            recv_sem=home_recv.at[o],
            device_id=z_dev(source_of(o)),
            device_id_type=MESH,
        )

    def mixer():
        await_bytes(att_in, att_recv)
        loads[3].wait()

        def tile(j, _):
            cols = pl.ds(pl.multiple_of(j * 256, 256), 256)
            total = jnp.zeros((chunk, 256), F32)
            for s in range(n_tp):
                total = total + jnp.dot(
                    att_in[s], mix[s * width_q : s * width_q + width_q, cols], preferred_element_type=F32
                )
            mixer_ref[:, cols] = total.astype(BF16)
            return 0

        lax.fori_loop(0, width // 256, tile, 0)

    dispatch(0)
    lax.fori_loop(0, rows_here // 128, place_own, 0)
    for copy in halos:
        copy.wait()
    place(halo[0], halo[1], 0, WINDOW)
    place(halo[2], halo[3], WINDOW + rows_here, WINDOW)
    share_of = blocks // n_z
    lax.fori_loop(0, 2 * share_of, attend, 0)
    for o in range(1, 2):
        dispatch(o)
    lax.fori_loop(2 * share_of, blocks, attend, 0)
    send_heads()
    for load in loads[:3]:
        load.wait()
    experts(0)
    for o in range(2, n_z):
        dispatch(o)
        experts(o - 1)
    combine(1)
    experts(n_z - 1)
    mixer()
    for o in range(2, n_z):
        combine(o)
    combine(0)

    for o in range(1, n_z):
        rt_copy(o).wait_send()
        z_copy(o).wait_send()
        home_copy(o).wait()
    for b in range(n_z):
        gone = pl.ds(0, (plane - 1) * capacity)
        await_bytes(outgoing.at[b, gone], out_send.at[b])
        await_bytes(produced.at[b, gone], back_send.at[b])
    await_bytes(att.at[pl.ds(0, (n_tp - 1) * chunk)], att_send)

    for part in range(tok // 32):
        rows = slice(part * 32, part * 32 + 32)
        total = partial[0, rows, :].astype(F32)
        for o in range(1, n_z):
            total = total + home[o, rows, :].astype(F32)
        expert_ref[rows, :] = total.astype(BF16)


def body(
    queries,
    key_heads,
    value_heads,
    sink_logits,
    mix_weight,
    expert_input,
    norm_gain,
    routes,
    route_weights,
    gate_weight,
    up_weight,
    down_weight,
):
    n_z, n_x, n_tp = lax.axis_size("zz"), lax.axis_size("xx"), lax.axis_size("tp")
    n_ep = n_z * n_x
    plane = n_x * n_tp
    rows_here, width_q = queries.shape
    kv_local = key_heads.shape[1] // HEAD_DIM
    tok, top_count = routes.shape
    capacity = 2 * tok * top_count // (n_ep * n_tp)
    slots = plane * capacity
    width = expert_input.shape[1]
    hidden = gate_weight.shape[2]
    first = lax.axis_index(("zz", "xx")) * rows_here
    cosines, sines = angle_tables(first - WINDOW, rows_here + 2 * WINDOW)
    routing = jnp.concatenate([routes.astype(F32), route_weights], axis=1).T
    vmem = pl.BlockSpec(memory_space=pltpu.VMEM)
    smem = pl.BlockSpec(memory_space=pltpu.SMEM)
    anywhere = pl.BlockSpec(memory_space=pl.ANY)
    reach = rows_here + 2 * WINDOW
    dma = pltpu.SemaphoreType.DMA
    return pl.pallas_call(
        functools.partial(kernel, (n_z, n_x, n_tp, top_count, capacity)),
        in_specs=[smem] + [vmem] * 8 + [anywhere] * 4,
        out_specs=[vmem, vmem],
        out_shape=[
            jax.ShapeDtypeStruct((rows_here // n_tp, width), BF16),
            jax.ShapeDtypeStruct((tok, width), BF16),
        ],
        scratch_shapes=[
            pltpu.VMEM((kv_local, reach, HEAD_DIM), BF16),
            pltpu.VMEM((kv_local, reach, HEAD_DIM), BF16),
            pltpu.VMEM((4, WINDOW, key_heads.shape[1]), BF16),
            pltpu.VMEM((rows_here, width_q), BF16),
            pltpu.VMEM((n_tp, rows_here // n_tp, width_q), BF16),
            pltpu.VMEM((n_z, 2 * top_count, tok), F32),
            pltpu.VMEM((n_z, tok, width), BF16),
            pltpu.VMEM((n_z, slots, width), BF16),
            pltpu.VMEM((n_z, slots, width), BF16),
            pltpu.VMEM((n_z, slots, width), BF16),
            pltpu.VMEM((n_z, slots, width), BF16),
            pltpu.VMEM((n_z, 2, tok, slots), BF16),
            pltpu.VMEM((n_z, tok, width), BF16),
            pltpu.VMEM((n_z, tok, width), BF16),
            pltpu.VMEM((width, hidden), BF16),
            pltpu.VMEM((width, hidden), BF16),
            pltpu.VMEM((hidden, width), BF16),
            pltpu.VMEM(mix_weight.shape, BF16),
            pltpu.VMEM((slots, hidden), BF16),
            dma((n_z,)),
            dma((n_z,)),
            dma((n_z,)),
            dma((n_z,)),
            dma((n_z,)),
            dma((n_z,)),
            dma((n_z,)),
            dma((n_z,)),
            dma((n_z,)),
            dma((n_z,)),
            dma,
            dma,
            dma((4,)),
            dma((4,)),
            dma((4,)),
        ],
        compiler_params=pltpu.CompilerParams(
            collective_id=0, has_side_effects=True, vmem_limit_bytes=67043328
        ),
        name="layer",
    )(
        sink_logits,
        routing,
        expert_input,
        norm_gain[None, :],
        queries,
        key_heads,
        value_heads,
        cosines,
        sines,
        gate_weight,
        up_weight,
        down_weight,
        mix_weight,
    )


def z_count(mesh, n_ep):
    coords = {getattr(d, "coords", (0, 0, 0))[2] for d in mesh.devices.flat}
    return len(coords) if n_ep % len(coords) == 0 else 1


def solution(mesh):
    n_ep, n_tp = mesh.shape["ep"], mesh.shape["tp"]
    n_z = z_count(mesh, n_ep)
    grid = Mesh(mesh.devices.reshape(n_z, n_ep // n_z, n_tp), ("zz", "xx", "tp"))
    ep = ("zz", "xx")
    every = ("zz", "xx", "tp")
    return jax.shard_map(
        body,
        mesh=grid,
        in_specs=(
            P(ep, "tp"),
            P(ep, "tp"),
            P(ep, "tp"),
            P("tp"),
            P(),
            P(every, None),
            P(),
            P(every, None),
            P(every, None),
            P(every, None, None),
            P(every, None, None),
            P(every, None, None),
        ),
        out_specs=(P(every, None), P(every, None)),
        check_vma=False,
    )
```

```python
import functools
import math

import jax
import jax.numpy as jnp
from jax import lax
from jax.experimental import pallas as pl
from jax.experimental.pallas import tpu as pltpu
from jax.sharding import Mesh
from jax.sharding import PartitionSpec as P

HEAD_DIM = 64
WINDOW = 128
GRID_W = 64
ROPE_BASE = 10000.0
CLAMP_LIMIT = 7.0
GATE_SLOPE = 1.702
NORM_EPS = 1e-05

F32 = jnp.float32
BF16 = jnp.bfloat16


def angle_tables(first, rows):
    half = HEAD_DIM // 2
    quarter = HEAD_DIM // 4
    lane = jnp.arange(2 * HEAD_DIM, dtype=jnp.int32) % HEAD_DIM
    freqs = ROPE_BASE ** (-jnp.arange(0, half, 2, dtype=F32) / half)
    lane_freq = jnp.tile(freqs, 2 * HEAD_DIM // quarter)
    by_row = (first // GRID_W + jnp.arange(rows // GRID_W, dtype=jnp.int32)).astype(F32)
    by_col = (jnp.arange(WINDOW, dtype=jnp.int32) % GRID_W).astype(F32)
    angle = jnp.concatenate([by_row, by_col])[:, None] * lane_freq[None, :]
    sign = jnp.where(lane % half < quarter, -1.0, 1.0).astype(F32)
    return jnp.cos(angle), jnp.sin(angle) * sign[None, :]


def turn(cells, cosines, sines):
    quarter = HEAD_DIM // 4
    width = cells.shape[1]
    lane = lax.broadcasted_iota(jnp.int32, cells.shape, 1)
    ahead = pltpu.roll(cells, width - quarter, 1)
    behind = pltpu.roll(cells, quarter, 1)
    partner = jnp.where(lane % (2 * quarter) < quarter, ahead, behind)
    return cells * cosines + partner * sines

MESH = pl.DeviceIdType.MESH


def kernel(
    sizes,
    sink,
    route_ref,
    x_ref,
    gain_ref,
    q_ref,
    k_ref,
    v_ref,
    cos_ref,
    sin_ref,
    wg_hbm,
    wu_hbm,
    wd_hbm,
    mix_hbm,
    mixer_ref,
    expert_ref,
    k_scr,
    v_scr,
    halo,
    att,
    att_in,
    routing,
    normed,
    outgoing,
    arrived,
    produced,
    returned,
    shares,
    partial,
    home,
    wg,
    wu,
    wd,
    mix,
    act,
    z_send,
    z_recv,
    rt_send,
    rt_recv,
    out_send,
    out_recv,
    back_send,
    back_recv,
    home_send,
    home_recv,
    att_send,
    att_recv,
    halo_send,
    halo_recv,
    load_sem,
):
    n_z, n_x, n_tp, top_count, capacity = sizes
    n_ep = n_z * n_x
    plane = n_x * n_tp
    slots = plane * capacity
    z, x, t = lax.axis_index("zz"), lax.axis_index("xx"), lax.axis_index("tp")
    me = x * n_tp + t
    ep = z * n_x + x
    rows_here, width_q = q_ref.shape
    tok, width = x_ref.shape
    length = rows_here * n_ep
    kv_local = k_scr.shape[0]
    bq = WINDOW
    span = bq + 2 * WINDOW
    blocks = rows_here // bq
    chunk = rows_here // n_tp

    def z_dev(b):
        return (b, x, t)

    def plane_dev(p):
        return (z, lax.div(p, n_tp), lax.rem(p, n_tp))

    def ep_dev(e):
        return (lax.div(e, n_x), lax.rem(e, n_x), t)

    after, before = lax.rem(ep + 1, n_ep), lax.rem(ep + n_ep - 1, n_ep)

    loads = [
        pltpu.make_async_copy(wg_hbm.at[0], wg, load_sem.at[0]),
        pltpu.make_async_copy(wu_hbm.at[0], wu, load_sem.at[1]),
        pltpu.make_async_copy(wd_hbm.at[0], wd, load_sem.at[2]),
        pltpu.make_async_copy(mix_hbm, mix, load_sem.at[3]),
    ]
    for load in loads:
        load.start()

    barrier = pltpu.get_barrier_semaphore()

    def greet_z(o, _):
        pl.semaphore_signal(barrier, inc=1, device_id=z_dev(lax.rem(z + o, n_z)), device_id_type=MESH)
        return 0

    def greet_plane(p, _):
        pl.semaphore_signal(
            barrier, inc=1, device_id=plane_dev(lax.rem(me + p, plane)), device_id_type=MESH
        )
        return 0

    lax.fori_loop(1, n_z, greet_z, 0)
    lax.fori_loop(1, plane, greet_plane, 0)
    for e in (after, before):
        pl.semaphore_signal(barrier, inc=1, device_id=ep_dev(e), device_id_type=MESH)

    for part in range(tok // 32):
        rows = slice(part * 32, part * 32 + 32)
        values = x_ref[rows, :].astype(F32)
        center = jnp.mean(values, axis=1, keepdims=True)
        spread = jnp.mean(jnp.square(values - center), axis=1, keepdims=True)
        normed[z, rows, :] = (
            (values - center) * lax.rsqrt(spread + NORM_EPS) * gain_ref[...]
        ).astype(BF16)
    routing[z] = route_ref[...]
    pl.semaphore_wait(barrier, n_z - 1 + plane - 1 + 2)

    def rt_copy(o):
        return pltpu.make_async_remote_copy(
            src_ref=routing.at[z],
            dst_ref=routing.at[z],
            send_sem=rt_send.at[o],
            recv_sem=rt_recv.at[z],
            device_id=z_dev(lax.rem(z + o, n_z)),
            device_id_type=MESH,
        )

    def z_copy(o):
        return pltpu.make_async_remote_copy(
            src_ref=normed.at[z],
            dst_ref=normed.at[z],
            send_sem=z_send.at[o],
            recv_sem=z_recv.at[z],
            device_id=z_dev(lax.rem(z + o, n_z)),
            device_id_type=MESH,
        )

    def halo_copy(source, which, start, target):
        return pltpu.make_async_remote_copy(
            src_ref=source.at[pl.ds(start, WINDOW)],
            dst_ref=halo.at[which],
            send_sem=halo_send.at[which],
            recv_sem=halo_recv.at[which],
            device_id=ep_dev(target),
            device_id_type=MESH,
        )

    halos = [
        halo_copy(k_ref, 0, rows_here - WINDOW, after),
        halo_copy(v_ref, 1, rows_here - WINDOW, after),
        halo_copy(k_ref, 2, 0, before),
        halo_copy(v_ref, 3, 0, before),
    ]
    for o in range(1, n_z):
        rt_copy(o).start()
    for copy in halos:
        copy.start()
    for o in range(1, n_z):
        z_copy(o).start()

    def await_bytes(ref, sem):
        pltpu.make_async_copy(ref, ref, sem).wait()

    def source_of(o):
        return lax.rem(z + n_z - o, n_z)

    slot_row = lax.broadcasted_iota(jnp.int32, (slots, tok), 0)
    lane_expert = (z * plane + lax.div(slot_row, capacity)).astype(F32)
    place_in = lax.rem(slot_row, capacity).astype(F32)
    upper = (
        lax.broadcasted_iota(jnp.int32, (tok, tok), 0) < lax.broadcasted_iota(jnp.int32, (tok, tok), 1)
    ).astype(F32).astype(BF16)

    def dispatch(o):
        b = source_of(o)
        if o > 0:
            await_bytes(routing.at[b], rt_recv.at[b])
            await_bytes(normed.at[b], z_recv.at[b])
        route = routing[b]
        member = jnp.zeros((slots, tok), F32)
        share = jnp.zeros((slots, tok), F32)
        for k in range(top_count):
            hit = route[k : k + 1, :] == lane_expert
            member = jnp.where(hit, 1.0, member)
            share = jnp.where(hit, route[top_count + k : top_count + k + 1, :], share)
        rank = jnp.dot(member.astype(BF16), upper, preferred_element_type=F32)
        pick = jnp.where(rank == place_in, member, 0.0)
        scaled = (share * pick).T
        coarse = scaled.astype(BF16)
        shares[b, 0] = coarse
        shares[b, 1] = (scaled - coarse.astype(F32)).astype(BF16)
        pick = pick.astype(BF16)

        def tile(j, _):
            cols = pl.ds(pl.multiple_of(j * 256, 256), 256)
            outgoing[b, :, cols] = jnp.dot(
                pick, normed[b, :, cols], preferred_element_type=F32
            ).astype(BF16)
            return 0

        lax.fori_loop(0, width // 256, tile, 0)
        exchange(outgoing, arrived, out_send, out_recv, b)

    def exchange(source, target, send, recv, b):
        mine = pl.ds(pl.multiple_of(me * capacity, capacity), capacity)

        def one(p, _):
            to = lax.rem(me + p, plane)
            pltpu.make_async_remote_copy(
                src_ref=source.at[b, pl.ds(pl.multiple_of(to * capacity, capacity), capacity)],
                dst_ref=target.at[b, mine],
                send_sem=send.at[b],
                recv_sem=recv.at[b],
                device_id=plane_dev(to),
                device_id_type=MESH,
            ).start()
            return 0

        lax.fori_loop(1, plane, one, 0)
        pltpu.make_async_copy(source.at[b, mine], target.at[b, mine], recv.at[b]).start()

    grid_rows = cos_ref.shape[0] - WINDOW
    of_row = lax.rem(lax.broadcasted_iota(jnp.int32, (WINDOW, 128), 1), HEAD_DIM) < HEAD_DIM // 2

    def angles(ref, at):
        start = lax.div(at, GRID_W)
        parts = [
            jnp.broadcast_to(ref[pl.ds(start + i, 1), :], (GRID_W, 128)) for i in range(WINDOW // GRID_W)
        ]
        return jnp.where(of_row, jnp.concatenate(parts, axis=0), ref[grid_rows:, :])

    def place(source, values, at, count):
        cosines, sines = angles(cos_ref, at), angles(sin_ref, at)
        for pair in range(kv_local // 2):
            cols = slice(pair * 128, pair * 128 + 128)
            turned = turn(source[:, cols].astype(F32), cosines, sines).astype(BF16)
            piece = values[:, cols]
            for side in range(2):
                lanes = slice(side * 64, side * 64 + 64)
                k_scr[2 * pair + side, pl.ds(at, count), :] = turned[:, lanes]
                v_scr[2 * pair + side, pl.ds(at, count), :] = piece[:, lanes]

    def place_own(i, _):
        at = pl.multiple_of(i * 128, 128)
        place(k_ref[pl.ds(at, 128), :], v_ref[pl.ds(at, 128), :], WINDOW + at, 128)
        return 0

    row = lax.rem(lax.broadcasted_iota(jnp.int32, (2 * bq, span), 0), bq)
    col = lax.broadcasted_iota(jnp.int32, (2 * bq, span), 1)
    top = lax.broadcasted_iota(jnp.int32, (2 * bq, 1), 0) < bq

    def attend(block, _):
        first = pl.multiple_of(block * bq, bq)
        cosines = angles(cos_ref, first + WINDOW) * HEAD_DIM**-0.5
        sines = angles(sin_ref, first + WINDOW) * HEAD_DIM**-0.5
        key_pos = ep * rows_here + first - WINDOW + col
        inside = (col >= row) & (col <= row + 2 * WINDOW) & (key_pos >= 0) & (key_pos < length)
        for g in range(kv_local):
            q = q_ref[pl.ds(first, bq), g * 128 : g * 128 + 128].astype(F32)
            q = turn(q, cosines, sines).astype(BF16)
            q2 = jnp.concatenate([q[:, :64], q[:, 64:]], axis=0)
            k = k_scr[g, pl.ds(first, span), :]
            v = v_scr[g, pl.ds(first, span), :]
            scores = lax.dot_general(q2, k, (((1,), (1,)), ((), ())), preferred_element_type=F32)
            scores = jnp.where(inside, scores, -jnp.inf)
            logit = jnp.where(top, sink[2 * g], sink[2 * g + 1])
            peak = jnp.maximum(jnp.max(scores, axis=1, keepdims=True), logit)
            weights = jnp.exp(scores - peak)
            total = jnp.sum(weights, axis=1, keepdims=True) + jnp.exp(logit - peak)
            chances = (weights * (1.0 / total)).astype(BF16)
            blend = jnp.dot(chances, v, preferred_element_type=F32).astype(BF16)
            att[pl.ds(first, bq), g * 128 : g * 128 + 128] = jnp.concatenate(
                [blend[:bq], blend[bq:]], axis=1
            )
        return 0

    def send_heads():
        def one(p, _):
            to = lax.rem(t + p, n_tp)
            pltpu.make_async_remote_copy(
                src_ref=att.at[pl.ds(pl.multiple_of(to * chunk, chunk), chunk)],
                dst_ref=att_in.at[t],
                send_sem=att_send,
                recv_sem=att_recv,
                device_id=(z, x, to),
                device_id_type=MESH,
            ).start()
            return 0

        lax.fori_loop(1, n_tp, one, 0)
        own = pl.ds(pl.multiple_of(t * chunk, chunk), chunk)
        pltpu.make_async_copy(att.at[own], att_in.at[t], att_recv).start()

    def experts(o):
        b = source_of(o)
        await_bytes(arrived.at[b], out_recv.at[b])
        hidden = wg.shape[1]

        def up(j, _):
            cols = pl.ds(pl.multiple_of(j * 256, 256), 256)
            rows = arrived[b]
            gate = jnp.dot(rows, wg[:, cols], preferred_element_type=F32)
            lift = jnp.dot(rows, wu[:, cols], preferred_element_type=F32)
            gate = jnp.minimum(gate, CLAMP_LIMIT)
            lift = jnp.clip(lift, -CLAMP_LIMIT, CLAMP_LIMIT)
            act[:, cols] = ((lift + 1.0) * gate * jax.nn.sigmoid(GATE_SLOPE * gate)).astype(BF16)
            return 0

        def down(j, _):
            cols = pl.ds(pl.multiple_of(j * 256, 256), 256)
            produced[b, :, cols] = jnp.dot(
                act[...], wd[:, cols], preferred_element_type=F32
            ).astype(BF16)
            return 0

        lax.fori_loop(0, hidden // 256, up, 0)
        lax.fori_loop(0, width // 256, down, 0)

    def send_back(o):
        exchange(produced, returned, back_send, back_recv, source_of(o))

    def combine(o):
        b = source_of(o)
        await_bytes(returned.at[b], back_recv.at[b])

        def tile(j, _):
            cols = pl.ds(pl.multiple_of(j * 256, 256), 256)
            rows = returned[b, :, cols]
            total = jnp.dot(shares[b, 0], rows, preferred_element_type=F32)
            total = total + jnp.dot(shares[b, 1], rows, preferred_element_type=F32)
            partial[o, :, cols] = total.astype(BF16)
            return 0

        lax.fori_loop(0, width // 256, tile, 0)
        if o > 0:
            home_copy(o).start()

    def home_copy(o):
        return pltpu.make_async_remote_copy(
            src_ref=partial.at[o],
            dst_ref=home.at[o],
            send_sem=home_send.at[o],
            recv_sem=home_recv.at[o],
            device_id=z_dev(source_of(o)),
            device_id_type=MESH,
        )

    def mixer():
        await_bytes(att_in, att_recv)
        loads[3].wait()

        def tile(j, _):
            cols = pl.ds(pl.multiple_of(j * 256, 256), 256)
            total = jnp.zeros((chunk, 256), F32)
            for s in range(n_tp):
                total = total + jnp.dot(
                    att_in[s], mix[s * width_q : s * width_q + width_q, cols], preferred_element_type=F32
                )
            mixer_ref[:, cols] = total.astype(BF16)
            return 0

        lax.fori_loop(0, width // 256, tile, 0)

    dispatch(0)
    lax.fori_loop(0, rows_here // 128, place_own, 0)
    for copy in halos:
        copy.wait()
    place(halo[0], halo[1], 0, WINDOW)
    place(halo[2], halo[3], WINDOW + rows_here, WINDOW)
    share_of = blocks // n_z
    lax.fori_loop(0, 2 * share_of, attend, 0)
    for o in range(1, 2):
        dispatch(o)
    lax.fori_loop(2 * share_of, blocks, attend, 0)
    send_heads()
    for load in loads[:3]:
        load.wait()
    experts(0)
    for o in range(2, n_z):
        dispatch(o)
        experts(o - 1)
        send_back(o - 1)
    if n_z > 2:
        combine(1)
    mixer()
    experts(n_z - 1)
    send_back(n_z - 1)
    send_back(0)
    for o in range(2 if n_z > 2 else 1, n_z):
        combine(o)
    combine(0)

    for o in range(1, n_z):
        rt_copy(o).wait_send()
        z_copy(o).wait_send()
        home_copy(o).wait()
    for b in range(n_z):
        gone = pl.ds(0, (plane - 1) * capacity)
        await_bytes(outgoing.at[b, gone], out_send.at[b])
        await_bytes(produced.at[b, gone], back_send.at[b])
    await_bytes(att.at[pl.ds(0, (n_tp - 1) * chunk)], att_send)

    for part in range(tok // 32):
        rows = slice(part * 32, part * 32 + 32)
        total = partial[0, rows, :].astype(F32)
        for o in range(1, n_z):
            total = total + home[o, rows, :].astype(F32)
        expert_ref[rows, :] = total.astype(BF16)


def body(
    queries,
    key_heads,
    value_heads,
    sink_logits,
    mix_weight,
    expert_input,
    norm_gain,
    routes,
    route_weights,
    gate_weight,
    up_weight,
    down_weight,
):
    n_z, n_x, n_tp = lax.axis_size("zz"), lax.axis_size("xx"), lax.axis_size("tp")
    n_ep = n_z * n_x
    plane = n_x * n_tp
    rows_here, width_q = queries.shape
    kv_local = key_heads.shape[1] // HEAD_DIM
    tok, top_count = routes.shape
    capacity = 2 * tok * top_count // (n_ep * n_tp)
    slots = plane * capacity
    width = expert_input.shape[1]
    hidden = gate_weight.shape[2]
    first = lax.axis_index(("zz", "xx")) * rows_here
    cosines, sines = angle_tables(first - WINDOW, rows_here + 2 * WINDOW)
    routing = jnp.concatenate([routes.astype(F32), route_weights], axis=1).T
    vmem = pl.BlockSpec(memory_space=pltpu.VMEM)
    smem = pl.BlockSpec(memory_space=pltpu.SMEM)
    anywhere = pl.BlockSpec(memory_space=pl.ANY)
    reach = rows_here + 2 * WINDOW
    dma = pltpu.SemaphoreType.DMA
    return pl.pallas_call(
        functools.partial(kernel, (n_z, n_x, n_tp, top_count, capacity)),
        in_specs=[smem] + [vmem] * 8 + [anywhere] * 4,
        out_specs=[vmem, vmem],
        out_shape=[
            jax.ShapeDtypeStruct((rows_here // n_tp, width), BF16),
            jax.ShapeDtypeStruct((tok, width), BF16),
        ],
        scratch_shapes=[
            pltpu.VMEM((kv_local, reach, HEAD_DIM), BF16),
            pltpu.VMEM((kv_local, reach, HEAD_DIM), BF16),
            pltpu.VMEM((4, WINDOW, key_heads.shape[1]), BF16),
            pltpu.VMEM((rows_here, width_q), BF16),
            pltpu.VMEM((n_tp, rows_here // n_tp, width_q), BF16),
            pltpu.VMEM((n_z, 2 * top_count, tok), F32),
            pltpu.VMEM((n_z, tok, width), BF16),
            pltpu.VMEM((n_z, slots, width), BF16),
            pltpu.VMEM((n_z, slots, width), BF16),
            pltpu.VMEM((n_z, slots, width), BF16),
            pltpu.VMEM((n_z, slots, width), BF16),
            pltpu.VMEM((n_z, 2, tok, slots), BF16),
            pltpu.VMEM((n_z, tok, width), BF16),
            pltpu.VMEM((n_z, tok, width), BF16),
            pltpu.VMEM((width, hidden), BF16),
            pltpu.VMEM((width, hidden), BF16),
            pltpu.VMEM((hidden, width), BF16),
            pltpu.VMEM(mix_weight.shape, BF16),
            pltpu.VMEM((slots, hidden), BF16),
            dma((n_z,)),
            dma((n_z,)),
            dma((n_z,)),
            dma((n_z,)),
            dma((n_z,)),
            dma((n_z,)),
            dma((n_z,)),
            dma((n_z,)),
            dma((n_z,)),
            dma((n_z,)),
            dma,
            dma,
            dma((4,)),
            dma((4,)),
            dma((4,)),
        ],
        compiler_params=pltpu.CompilerParams(
            collective_id=0, has_side_effects=True, vmem_limit_bytes=67043328
        ),
        name="layer",
    )(
        sink_logits,
        routing,
        expert_input,
        norm_gain[None, :],
        queries,
        key_heads,
        value_heads,
        cosines,
        sines,
        gate_weight,
        up_weight,
        down_weight,
        mix_weight,
    )


def z_count(mesh, n_ep):
    coords = {getattr(d, "coords", (0, 0, 0))[2] for d in mesh.devices.flat}
    return len(coords) if n_ep % len(coords) == 0 else 1


def solution(mesh):
    n_ep, n_tp = mesh.shape["ep"], mesh.shape["tp"]
    n_z = z_count(mesh, n_ep)
    grid = Mesh(mesh.devices.reshape(n_z, n_ep // n_z, n_tp), ("zz", "xx", "tp"))
    ep = ("zz", "xx")
    every = ("zz", "xx", "tp")
    return jax.shard_map(
        body,
        mesh=grid,
        in_specs=(
            P(ep, "tp"),
            P(ep, "tp"),
            P(ep, "tp"),
            P("tp"),
            P(),
            P(every, None),
            P(),
            P(every, None),
            P(every, None),
            P(every, None, None),
            P(every, None, None),
            P(every, None, None),
        ),
        out_specs=(P(every, None), P(every, None)),
        check_vma=False,
    )
```
